32 devices in a mesh: grp: 2 (over x), ep: 16 (over z, y, core).
Axes of the slice: x: 2, y: 2, z: 4, core: 2. Of those that a mesh axis runs over, the one named last changes fastest.
Arguments:
- tokens: bfloat16 [1024, 2048], P(('grp', 'ep')), parts along dimension 0, may hold values from -6 to 6
- norm_gain: float32 [2048], replicated, may hold values from 0.1 to 1.9
- routing: int32 [1024, 8], P(('grp', 'ep')), parts along dimension 0, may hold values from 0 to 15, all different within a row; in each aligned block of 32 rows (0 to 31, 32 to 63, ...) at most 32 rows name the same one
- gates: float32 [1024, 8], P(('grp', 'ep')), parts along dimension 0, may hold values from 0.05 to 0.6
- w_gate: bfloat16 [16, 2048, 512], P('ep'), may hold values from -0.125 to 0.125
- w_up: bfloat16 [16, 2048, 512], P('ep'), may hold values from -0.125 to 0.125
- w_down: bfloat16 [16, 512, 2048], P('ep'), may hold values from -0.25 to 0.25
- shared_gate: bfloat16 [2048, 512], replicated, may hold values from -0.125 to 0.125
- shared_up: bfloat16 [2048, 512], replicated, may hold values from -0.125 to 0.125
- shared_down: bfloat16 [512, 2048], replicated, may hold values from -0.25 to 0.25
Outputs:
- mixed: bfloat16 [1024, 2048], P(('grp', 'ep')), parts along dimension 0
The draws below stay inside these ranges and needn't reach their ends.
There are 2 independent parts, one for each index of `grp`. The reference program is written for one: setup_inputs(seed, part) draws one part's arguments, and reference() takes and returns one part's arrays. A program takes and returns all parts, laid end to end along the dimension named above; an argument that names none is the same for every part. Nothing has to cross between parts.
Inputs may be any that keep to these rules, and one draw needn't show every extreme that they name: `routing`: within the 32 rows of one device no expert is named by more than 32 rows, and in every draw some expert is named by exactly 32 rows of some device; each row names 8 different experts.
All inputs are finite; a program needn't handle non-finite values.
Results may differ from the reference program's by a relative error of at most 0.0067.
Values may be sent and summed in bfloat16 or wider, within the bound.
A program may use at most 128 MiB of HBM per device.

```python
import math
import jax
import jax.numpy as jnp
import numpy as np
from jax import lax

D = 2048
FF = 512
SHARED_FF = 512
TOP_K = 8
TOK_DEV = 32
EXPERTS = 16
TOKENS = 512
SLOTS = 32
N_EP = 16


def steps_of(key, extent, pieces, least, high):
    factor_of, own = 1.0, jax.random.fold_in(key, 6)
    for dim, shards_of in pieces:
        heights = jnp.exp(jax.random.uniform(jax.random.fold_in(own, dim), (shards_of,), jnp.float32, least / len(pieces), high / len(pieces)))
        factor_of = factor_of * jnp.repeat(heights, extent[dim] // shards_of).reshape([-1 if axis == dim else 1 for axis in range(len(extent))])
    return factor_of


def routed_block(key, own, number, rows, amount, top, reach, skew):
    ranking = jax.random.permutation(key, amount)
    crowded, common = load_shares(amount, rows * top, reach, skew, True), load_shares(amount, rows * top, reach, skew, False)
    places = jnp.arange(amount)

    def named(sizes, rotation):
        used = int((sizes > 0).sum())
        fixed = max(1, used // 4)
        passed = fixed + (places - fixed + rotation * (used - fixed)) % max(1, amount - fixed)
        return jnp.zeros((amount,), jnp.int32).at[ranking[jnp.where(places < fixed, places, passed)]].set(jnp.asarray(sizes, jnp.int32))

    sizes = jnp.where(number % 4 == 0, named(crowded, number // 4), named(common, number - number // 4 - 1))
    mixed = jax.random.permutation(jax.random.fold_in(own, 3), amount)
    giver, receiver = mixed[0:amount // 2 * 2:2], mixed[1:amount // 2 * 2:2]
    slack = jnp.minimum(sizes[giver] - 1, reach - sizes[receiver]) // 2
    slack = jnp.where((giver == ranking[0]) | (receiver == ranking[0]) | (sizes[receiver] == 0), 0, jnp.maximum(slack, 0))
    passed = jax.random.randint(jax.random.fold_in(own, 4), (amount // 2,), 0, 1 << 20) % (slack + 1)
    sizes = sizes.at[giver].add(-passed).at[receiver].add(passed)
    labels = jnp.searchsorted(jnp.cumsum(sizes), jnp.arange(rows * top), side="right").astype(jnp.int32)
    grid = labels.reshape(top, rows).T
    grid = grid[jax.random.permutation(jax.random.fold_in(own, 1), rows)]
    rotation = jax.random.randint(jax.random.fold_in(own, 2), (rows, 1), 0, top)
    return jnp.take_along_axis(grid, (jnp.arange(top)[None, :] + rotation) % top, axis=1)


def load_shares(amount, total, limit, skew, full):
    loads = [(1 << 20) // math.isqrt(standing ** skew) + 1 for standing in range(1, amount + 1)]
    largest = limit if full else min(limit, max(-(-total // amount), total * loads[0] // sum(loads)))
    least = 1 if total - largest >= amount - 1 else 0
    given, surplus = [largest] + [least] * (amount - 1), total - largest - least * (amount - 1)
    while surplus > 0:
        candidates = [i for i in range(1, amount) if given[i] < largest] or [i for i in range(1, amount) if given[i] < limit]
        mass, budget = sum([loads[i] for i in candidates]), surplus
        for i in candidates:
            more = min(limit - given[i], max(1, budget * loads[i] // mass), surplus)
            given[i] = given[i] + more
            surplus = surplus - more
    return np.array(given)


def bell_draw(own_key, shape, width, bound, split=(), kind=jnp.bfloat16):
    values = jax.random.normal(own_key, shape, jnp.float32) * width
    if len(split) > 0:
        values = steps_of(own_key, shape, split, -0.22, 0.18) * values
    return jnp.clip(values, min=-bound, max=bound).astype(kind)


def setup_inputs(seed: int = 0, part: int = 0) -> dict:
    key_of = jax.random.split(jax.random.key(seed), 11)
    own_keys = jax.random.split(jax.random.fold_in(key_of[10], part), 11)
    tokens = bell_draw(own_keys[0], (TOKENS, D), 1.0, 6.0, ((0, 16),))
    norm_gain = jnp.clip(1.0 + 0.18 * jax.random.normal(key_of[1], (D,), jnp.float32), 0.1, 1.9)
    routing_keys = jax.random.split(jax.random.fold_in(own_keys[2], 1), TOKENS // TOK_DEV)
    routing_turns = jax.random.permutation(jax.random.fold_in(own_keys[2], 3), TOKENS // TOK_DEV)
    routing = jax.vmap(lambda own, number: routed_block(jax.random.fold_in(own_keys[2], 2), own, number, TOK_DEV, EXPERTS, TOP_K, SLOTS, 2))(routing_keys, routing_turns).reshape((TOKENS, TOP_K))
    gates = jnp.clip(jnp.exp(math.log(0.6) - 2.4849067 * jax.random.uniform(own_keys[3], (TOKENS, TOP_K), jnp.float32) ** steps_of(own_keys[3], (TOKENS, TOP_K), ((0, 16),), -0.2, 0.2)), 0.05, 0.6)
    w_gate = bell_draw(key_of[4], (EXPERTS, D, FF), D ** -0.5, 0.125, ((0, 16),))
    w_up = bell_draw(key_of[5], (EXPERTS, D, FF), D ** -0.5, 0.125, ((0, 16),))
    w_down = bell_draw(key_of[6], (EXPERTS, FF, D), FF ** -0.5, 0.25, ((0, 16),))
    shared_gate = bell_draw(key_of[7], (D, SHARED_FF), D ** -0.5, 0.125)
    shared_up = bell_draw(key_of[8], (D, SHARED_FF), D ** -0.5, 0.125)
    shared_down = bell_draw(key_of[9], (SHARED_FF, D), SHARED_FF ** -0.5, 0.25)
    return dict(tokens=tokens, norm_gain=norm_gain, routing=routing, gates=gates, w_gate=w_gate, w_up=w_up, w_down=w_down, shared_gate=shared_gate, shared_up=shared_up, shared_down=shared_down)


epsilon = 1e-06

def rms_normed(tokens, norm_gain):
    floats = tokens.astype(jnp.float32)
    scale_inv = lax.rsqrt(lax.optimization_barrier(jnp.mean(floats * floats, axis=-1, keepdims=True)) + epsilon)
    return (floats * scale_inv * norm_gain.astype(jnp.float32)).astype(jnp.bfloat16)

def reference(tokens, norm_gain, routing, gates, w_gate, w_up, w_down, shared_gate, shared_up, shared_down):
    normed = rms_normed(tokens, norm_gain)
    shared_hidden = (jax.nn.silu(jnp.dot(normed, shared_gate, preferred_element_type=jnp.float32)) * jnp.dot(normed, shared_up, preferred_element_type=jnp.float32)).astype(jnp.bfloat16)
    shared_out = jnp.dot(shared_hidden, shared_down, preferred_element_type=jnp.float32)
    capacity = N_EP * SLOTS
    token_total = normed.shape[0]
    positions = jnp.arange(token_total, dtype=jnp.int32)

    def visit(totals, inputs):
        gate_part, up_part, down_part, expert = inputs
        chosen_pairs = routing == expert
        chosen = jnp.any(chosen_pairs, axis=1)
        weights = lax.optimization_barrier(jnp.sum(jnp.where(chosen_pairs, gates, jnp.zeros_like(gates)), axis=1))
        ranked = jnp.cumsum(chosen.astype(jnp.int32)) - 1
        target = jnp.where(chosen, ranked, capacity).astype(jnp.int32)
        picks = jnp.zeros((capacity,), jnp.int32).at[target].set(positions, mode='drop')
        live = jnp.zeros((capacity,), weights.dtype).at[target].set(weights, mode='drop')
        picked = normed[picks]
        hidden = (jax.nn.silu(jnp.dot(picked, gate_part, preferred_element_type=jnp.float32)) * jnp.dot(picked, up_part, preferred_element_type=jnp.float32)).astype(jnp.bfloat16)
        outputs = jnp.dot(hidden, down_part, preferred_element_type=jnp.float32).astype(jnp.bfloat16)
        totals = totals.at[picks].add(live[:, None] * outputs.astype(jnp.float32))
        return (totals, None)
    start = jnp.zeros((token_total, normed.shape[1]), jnp.float32)
    routed, _ = lax.scan(visit, start, (w_gate, w_up, w_down, jnp.arange(w_gate.shape[0], dtype=jnp.int32)))
    return (shared_out + routed).astype(jnp.bfloat16)
```

```python
import functools

import jax
import jax.numpy as jnp
from jax import lax
from jax.experimental import pallas as pl
from jax.experimental.pallas import tpu as pltpu
from jax.sharding import PartitionSpec as P

epsilon = 1e-06
MESH = pl.DeviceIdType.MESH
F32, BF16 = jnp.float32, jnp.bfloat16


def flipped(value, mask):
    bit = 1
    while bit <= mask:
        if mask & bit:
            value = value + bit * (1 - 2 * ((value // bit) % 2))
        bit *= 2
    return value


def silu(v):
    return v / (1.0 + jnp.exp(-v))


def dot(a, b):
    return jnp.dot(a, b, preferred_element_type=F32)


def kernel(
    zs, ys, tok_ref, gain_ref, routing_ref, gates_ref, wg_hbm, wu_hbm, wd_hbm, sg_hbm, su_hbm, sd_hbm,
    out_ref, buf, part, from_core, to_y, from_y, to_z, from_z, wg, wu, wd, sg, su, sd,
    w_sem, agz_s, agz_r, agy_s, agy_r, agc_s, agc_r, rsc_s, rsc_r, rsy_s, rsy_r, rsz_s, rsz_r,
):
    toks, width = tok_ref.shape
    top = routing_ref.shape[1]
    lanes = buf.shape[-1] - width
    n = zs * ys * 2
    me = lax.axis_index("ep")
    c = me % 2
    y = (me // 2) % ys
    z = me // (2 * ys)
    oc, oy = 1 - c, (y + 1) % ys

    def dev(zi, yi, ci):
        return {"ep": (zi * ys + yi) * 2 + ci}

    pairs = ((sg_hbm, sg), (su_hbm, su), (sd_hbm, sd), (wg_hbm, wg), (wu_hbm, wu), (wd_hbm, wd))
    loads = [pltpu.make_async_copy(a, b, w_sem.at[i]) for i, (a, b) in enumerate(pairs)]
    for load in loads:
        load.start()

    barrier = pltpu.get_barrier_semaphore()
    peers = [dev(flipped(z, k), y, c) for k in range(1, zs)] + [dev(z, oy, c), dev(z, y, oc)]
    for peer in peers:
        pl.semaphore_signal(barrier, inc=1, device_id=peer, device_id_type=MESH)

    floats = tok_ref[...].astype(F32)
    scale_inv = lax.rsqrt(jnp.mean(floats * floats, axis=-1, keepdims=True) + epsilon)
    normed = (floats * scale_inv * gain_ref[...]).astype(BF16)
    lane = lax.broadcasted_iota(jnp.int32, (toks, lanes), 1)
    weight = jnp.zeros((toks, lanes), F32)
    for k in range(top):
        named = (routing_ref[:, k : k + 1] == lane) | (routing_ref[:, k : k + 1] + n == lane)
        weight = weight + jnp.where(named, gates_ref[:, k : k + 1], 0.0)
    high = weight.astype(BF16).astype(F32)
    low = weight - high
    buf[z, c, y, :, :width] = normed
    buf[z, c, y, :, width:] = jnp.where(lane < n, high, low).astype(BF16)

    pl.semaphore_wait(barrier, len(peers))

    sent = []

    def send(src, dst, s_sem, r_sem, target):
        copy = pltpu.make_async_remote_copy(
            src_ref=src, dst_ref=dst, send_sem=s_sem, recv_sem=r_sem,
            device_id=target, device_id_type=MESH,
        )
        copy.start()
        sent.append(copy)

    def arrived(dst, s_sem, r_sem, source):
        pltpu.make_async_remote_copy(
            src_ref=dst, dst_ref=dst, send_sem=s_sem, recv_sem=r_sem,
            device_id=source, device_id_type=MESH,
        ).wait_recv()

    def forward_y(k):
        block = buf.at[flipped(z, k), c, y]
        send(block, block, agy_s.at[k], agy_r.at[k], dev(z, oy, c))

    def forward_core(k, yi, j):
        block = buf.at[flipped(z, k), c, yi]
        send(block, block, agc_s.at[k, j], agc_r.at[k, j], dev(z, y, oc))

    def take_z(k):
        arrived(buf.at[flipped(z, k), c, y], agz_s.at[k], agz_r.at[k], dev(flipped(z, k), y, c))
        forward_y(k)
        forward_core(k, y, 0)

    def take_y(k):
        arrived(buf.at[flipped(z, k), c, oy], agy_s.at[k], agy_r.at[k], dev(z, oy, c))
        forward_core(k, oy, 1)

    def experts(k):
        zi = flipped(z, k)
        for j, yi in ((0, y), (1, oy)):
            arrived(buf.at[zi, oc, yi], agc_s.at[k, j], agc_r.at[k, j], dev(z, y, oc))
        rows = 2 * ys * toks
        x = buf[zi, :, :, :, :width].reshape(rows, width)
        tags = buf[zi, :, :, :, width:].reshape(rows, lanes).astype(F32)
        where = lax.broadcasted_iota(jnp.int32, (rows, lanes), 1)
        mine = (where == me) | (where == me + n)
        scale = jnp.sum(jnp.where(mine, tags, 0.0), axis=-1, keepdims=True)
        hidden = (silu(dot(x, wg[0])) * dot(x, wu[0])).astype(BF16)
        outs = dot(hidden, wd[0]).astype(BF16).astype(F32) * scale
        part[zi] = outs.astype(BF16).reshape(2, ys, toks, width)
        send(part.at[zi, oc], from_core.at[k], rsc_s.at[k], rsc_r.at[k], dev(z, y, oc))

    def add_core(k):
        zi = flipped(z, k)
        arrived(from_core.at[k], rsc_s.at[k], rsc_r.at[k], dev(z, y, oc))
        both = part[zi, c, oy].astype(F32) + from_core[k, oy].astype(F32)
        to_y[k] = both.astype(BF16)
        send(to_y.at[k], from_y.at[k], rsy_s.at[k], rsy_r.at[k], dev(z, oy, c))

    def add_y(k):
        zi = flipped(z, k)
        arrived(from_y.at[k], rsy_s.at[k], rsy_r.at[k], dev(z, oy, c))
        total = part[zi, c, y].astype(F32) + from_core[k, y].astype(F32) + from_y[k].astype(F32)
        if k == 0:
            return total
        to_z[k] = total.astype(BF16)
        send(to_z.at[k], from_z.at[k], rsz_s.at[k], rsz_r.at[k], dev(zi, y, c))

    for k in range(1, zs):
        own = buf.at[z, c, y]
        send(own, own, agz_s.at[k], agz_r.at[k], dev(flipped(z, k), y, c))
    forward_y(0)
    forward_core(0, y, 0)

    for load in loads[:3]:
        load.wait()
    x = buf[z, c, y, :, :width]
    shared_hidden = (silu(dot(x, sg[...])) * dot(x, su[...])).astype(BF16)
    total = dot(shared_hidden, sd[...])
    for load in loads[3:]:
        load.wait()

    for i in range(zs):
        if i + 1 < zs:
            take_z(i + 1)
        take_y(i)
        experts(i)
        if i >= 1:
            add_core(i - 1)
        if i >= 2:
            got = add_y(i - 2)
            if i == 2:
                total = total + got
    add_core(zs - 1)
    for i in range(max(zs - 2, 0), zs):
        got = add_y(i)
        if i == 0:
            total = total + got
    for k in range(1, zs):
        arrived(from_z.at[k], rsz_s.at[k], rsz_r.at[k], dev(flipped(z, k), y, c))
        total = total + from_z[k].astype(F32)
    out_ref[...] = total.astype(BF16)
    for copy in sent:
        copy.wait_send()


def body(zs, ys, *args):
    tokens, norm_gain, routing, gates, w_gate, w_up, w_down, shared_gate, shared_up, shared_down = args
    toks, width = tokens.shape
    n = zs * ys * 2
    lanes = -(-2 * n // 128) * 128
    dma = pltpu.SemaphoreType.DMA
    vmem = pl.BlockSpec(memory_space=pltpu.VMEM)
    hbm = pl.BlockSpec(memory_space=pl.ANY)
    return pl.pallas_call(
        functools.partial(kernel, zs, ys),
        out_shape=jax.ShapeDtypeStruct((toks, width), BF16),
        in_specs=[vmem] * 4 + [hbm] * 6,
        out_specs=vmem,
        scratch_shapes=[
            pltpu.VMEM((zs, 2, ys, toks, width + lanes), BF16),
            pltpu.VMEM((zs, 2, ys, toks, width), BF16),
            pltpu.VMEM((zs, ys, toks, width), BF16),
            pltpu.VMEM((zs, toks, width), BF16),
            pltpu.VMEM((zs, toks, width), BF16),
            pltpu.VMEM((zs, toks, width), BF16),
            pltpu.VMEM((zs, toks, width), BF16),
        ]
        + [pltpu.VMEM(w.shape, BF16) for w in args[4:]]
        + [dma((6,))]
        + [dma((zs,))] * 4
        + [dma((zs, 2))] * 2
        + [dma((zs,))] * 6,
        compiler_params=pltpu.CompilerParams(
            collective_id=0, has_side_effects=True, vmem_limit_bytes=60 * 1024 * 1024
        ),
    )(tokens, norm_gain.reshape(1, width), *args[2:])


def solution(mesh):
    chips = mesh.shape["ep"] // 2
    ys = 2
    zs = chips // ys
    placed = (
        P(("grp", "ep"), None),
        P(),
        P(("grp", "ep"), None),
        P(("grp", "ep"), None),
        P("ep", None, None),
        P("ep", None, None),
        P("ep", None, None),
        P(),
        P(),
        P(),
    )
    return jax.shard_map(
        functools.partial(body, zs, ys),
        mesh=mesh,
        in_specs=placed,
        out_specs=P(("grp", "ep"), None),
        check_vma=False,
    )
```

```python
import functools

import jax
import jax.numpy as jnp
from jax import lax
from jax.experimental import pallas as pl
from jax.experimental.pallas import tpu as pltpu
from jax.sharding import PartitionSpec as P

epsilon = 1e-06
MESH = pl.DeviceIdType.MESH
F32, BF16 = jnp.float32, jnp.bfloat16


def flipped(value, mask):
    bit = 1
    while bit <= mask:
        if mask & bit:
            value = value + bit * (1 - 2 * ((value // bit) % 2))
        bit *= 2
    return value


def silu(v):
    return v / (1.0 + jnp.exp(-v))


def dot(a, b):
    return jnp.dot(a, b, preferred_element_type=F32)


def kernel(
    zs, ys, tok_ref, gain_ref, routing_ref, gates_ref, wg_hbm, wu_hbm, wd_hbm, sg_hbm, su_hbm, sd_hbm,
    out_ref, buf, part, from_core, to_y, from_y, to_z, from_z, sums, wg, wu, wd, sg, su, sd,
    w_sem, agz_s, agz_r, agy_s, agy_r, agc_s, agc_r, rsc_s, rsc_r, rsy_s, rsy_r, rsz_s, rsz_r,
):
    toks, width = tok_ref.shape
    top = routing_ref.shape[0]
    lanes = buf.shape[-1] - width
    n = zs * ys * 2
    me = lax.axis_index("ep")
    c = me % 2
    y = (me // 2) % ys
    z = me // (2 * ys)
    oc, oy = 1 - c, (y + 1) % ys

    def dev(zi, yi, ci):
        return {"ep": (zi * ys + yi) * 2 + ci}

    pairs = ((sg_hbm, sg), (su_hbm, su), (sd_hbm, sd), (wg_hbm, wg), (wu_hbm, wu), (wd_hbm, wd))
    loads = [pltpu.make_async_copy(a, b, w_sem.at[i]) for i, (a, b) in enumerate(pairs)]
    for load in loads:
        load.start()

    barrier = pltpu.get_barrier_semaphore()
    peers = [dev(flipped(z, k), y, c) for k in range(1, zs)] + [dev(z, oy, c), dev(z, y, oc)]
    for peer in peers:
        pl.semaphore_signal(barrier, inc=1, device_id=peer, device_id_type=MESH)

    floats = tok_ref[...].astype(F32)
    scale_inv = lax.rsqrt(jnp.mean(floats * floats, axis=-1, keepdims=True) + epsilon)
    normed = (floats * scale_inv * gain_ref[...]).astype(BF16)
    lane = lax.broadcasted_iota(jnp.int32, (toks, lanes), 1)
    tag = lax.broadcasted_iota(jnp.int32, (lanes, toks), 0)
    weight = jnp.zeros((lanes, toks), F32)
    for k in range(top):
        named = (routing_ref[k : k + 1, :] == tag) | (routing_ref[k : k + 1, :] + n == tag)
        weight = weight + jnp.where(named, gates_ref[k : k + 1, :], 0.0)
    weight = weight.T
    high = weight.astype(BF16).astype(F32)
    low = weight - high
    buf[z, c, y, :, :width] = normed
    buf[z, c, y, :, width:] = jnp.where(lane < n, high, low).astype(BF16)

    pl.semaphore_wait(barrier, len(peers))

    parts = 2 if toks % 32 == 0 else 1
    size = toks // parts
    gather_order = list(range(1, zs))
    sent = []

    def send(src, dst, s_sem, r_sem, target):
        copy = pltpu.make_async_remote_copy(
            src_ref=src, dst_ref=dst, send_sem=s_sem, recv_sem=r_sem,
            device_id=target, device_id_type=MESH,
        )
        copy.start()
        sent.append(copy)

    def piece(zi, ci, yi, h):
        return buf.at[zi, ci, yi, pl.ds(h * size, size)]

    def arrived(dst, s_sem, r_sem, source):
        pltpu.make_async_remote_copy(
            src_ref=dst, dst_ref=dst, send_sem=s_sem, recv_sem=r_sem,
            device_id=source, device_id_type=MESH,
        ).wait_recv()

    def forward_y(k, h):
        block = piece(flipped(z, k), c, y, h)
        send(block, block, agy_s.at[k, h], agy_r.at[k, h], dev(z, oy, c))

    def forward_core(k, yi, j, h):
        block = piece(flipped(z, k), c, yi, h)
        send(block, block, agc_s.at[k, j, h], agc_r.at[k, j, h], dev(z, y, oc))

    def take_z(k):
        for h in range(parts):
            arrived(piece(flipped(z, k), c, y, h), agz_s.at[k, h], agz_r.at[k, h], dev(flipped(z, k), y, c))
            forward_y(k, h)
            forward_core(k, y, 0, h)

    def take_y(k):
        for h in range(parts):
            arrived(piece(flipped(z, k), c, oy, h), agy_s.at[k, h], agy_r.at[k, h], dev(z, oy, c))
            forward_core(k, oy, 1, h)

    def experts(k):
        zi = flipped(z, k)
        for j, yi in ((0, y), (1, oy)):
            for h in range(parts):
                arrived(piece(zi, oc, yi, h), agc_s.at[k, j, h], agc_r.at[k, j, h], dev(z, y, oc))
        rows = 2 * ys * toks
        x = buf[zi, :, :, :, :width].reshape(rows, width)
        tags = buf[zi, :, :, :, width:].reshape(rows, lanes).astype(F32)
        where = lax.broadcasted_iota(jnp.int32, (rows, lanes), 1)
        mine = (where == me) | (where == me + n)
        scale = jnp.sum(jnp.where(mine, tags, 0.0), axis=-1, keepdims=True)
        hidden = (silu(dot(x, wg[0])) * dot(x, wu[0])).astype(BF16)
        outs = dot(hidden, wd[0]).astype(BF16).astype(F32) * scale
        part[zi] = outs.astype(BF16).reshape(2, ys, toks, width)
        for j, yi in ((0, oy), (1, y)):
            send(part.at[zi, oc, yi], from_core.at[k, yi], rsc_s.at[k, j], rsc_r.at[k, j], dev(z, y, oc))

    def add_core(k):
        zi = flipped(z, k)
        arrived(from_core.at[k, oy], rsc_s.at[k, 0], rsc_r.at[k, 0], dev(z, y, oc))
        for h in range(parts):
            at = pl.ds(h * size, size)
            both = part[zi, c, oy, at].astype(F32) + from_core[k, oy, at].astype(F32)
            to_y[k, at] = both.astype(BF16)
            send(to_y.at[k, at], from_y.at[k, at], rsy_s.at[k, h], rsy_r.at[k, h], dev(z, oy, c))

    def add_y(k):
        zi = flipped(z, k)
        arrived(from_core.at[k, y], rsc_s.at[k, 1], rsc_r.at[k, 1], dev(z, y, oc))
        for h in range(parts):
            at = pl.ds(h * size, size)
            arrived(from_y.at[k, at], rsy_s.at[k, h], rsy_r.at[k, h], dev(z, oy, c))
            total = part[zi, c, y, at].astype(F32) + from_core[k, y, at].astype(F32) + from_y[k, at].astype(F32)
            if k == 0:
                sums[at] = sums[at] + total
            else:
                to_z[k, at] = total.astype(BF16)
                send(to_z.at[k, at], from_z.at[k, at], rsz_s.at[k, h], rsz_r.at[k, h], dev(zi, y, c))

    for h in range(parts):
        forward_y(0, h)
        forward_core(0, y, 0, h)
    for k in gather_order:
        for h in range(parts):
            own = piece(z, c, y, h)
            send(own, own, agz_s.at[k, h], agz_r.at[k, h], dev(flipped(z, k), y, c))

    for load in loads[:3]:
        load.wait()
    x = buf[z, c, y, :, :width]
    shared_hidden = (silu(dot(x, sg[...])) * dot(x, su[...])).astype(BF16)
    sums[...] = dot(shared_hidden, sd[...])
    for load in loads[3:]:
        load.wait()

    def program():
        for i in range(zs):
            if i + 1 < zs:
                yield take_z, i + 1
            yield take_y, i
            yield experts, i
            if i == zs - 2:
                for k in range(zs - 2, 0, -1):
                    yield add_core, k
        yield add_core, zs - 1
        yield add_core, 0
        for k in range(zs - 2, 0, -1):
            yield add_y, k
        yield add_y, zs - 1
        yield add_y, 0

    for step, k in program():
        step(k)
    total = sums[...]
    for k in gather_order:
        for h in range(parts):
            at = pl.ds(h * size, size)
            arrived(from_z.at[k, at], rsz_s.at[k, h], rsz_r.at[k, h], dev(flipped(z, k), y, c))
        total = total + from_z[k].astype(F32)
    out_ref[...] = total.astype(BF16)
    for copy in sent:
        copy.wait_send()


def body(zs, ys, *args):
    tokens, norm_gain, routing, gates, w_gate, w_up, w_down, shared_gate, shared_up, shared_down = args
    toks, width = tokens.shape
    n = zs * ys * 2
    lanes = -(-2 * n // 128) * 128
    dma = pltpu.SemaphoreType.DMA
    vmem = pl.BlockSpec(memory_space=pltpu.VMEM)
    hbm = pl.BlockSpec(memory_space=pl.ANY)
    return pl.pallas_call(
        functools.partial(kernel, zs, ys),
        out_shape=pltpu.VMEM((toks, width), BF16),
        in_specs=[vmem] * 4 + [hbm] * 6,
        out_specs=vmem,
        scratch_shapes=[
            pltpu.VMEM((zs, 2, ys, toks, width + lanes), BF16),
            pltpu.VMEM((zs, 2, ys, toks, width), BF16),
            pltpu.VMEM((zs, ys, toks, width), BF16),
            pltpu.VMEM((zs, toks, width), BF16),
            pltpu.VMEM((zs, toks, width), BF16),
            pltpu.VMEM((zs, toks, width), BF16),
            pltpu.VMEM((zs, toks, width), BF16),
            pltpu.VMEM((toks, width), F32),
        ]
        + [pltpu.VMEM(w.shape, BF16) for w in args[4:]]
        + [dma((6,))]
        + [dma((zs, 2))] * 4
        + [dma((zs, 2, 2))] * 2
        + [dma((zs, 2))] * 6,
        compiler_params=pltpu.CompilerParams(
            collective_id=0, has_side_effects=True, vmem_limit_bytes=60 * 1024 * 1024
        ),
    )(tokens, norm_gain.reshape(1, width), routing.T, gates.T, *args[4:])


def solution(mesh):
    chips = mesh.shape["ep"] // 2
    ys = 2
    zs = chips // ys
    placed = (
        P(("grp", "ep"), None),
        P(),
        P(("grp", "ep"), None),
        P(("grp", "ep"), None),
        P("ep", None, None),
        P("ep", None, None),
        P("ep", None, None),
        P(),
        P(),
        P(),
    )
    return jax.shard_map(
        functools.partial(body, zs, ys),
        mesh=mesh,
        in_specs=placed,
        out_specs=P(("grp", "ep"), None),
        check_vma=False,
    )
```

```python
import functools

import jax
import jax.numpy as jnp
from jax import lax
from jax.experimental import pallas as pl
from jax.experimental.pallas import tpu as pltpu
from jax.sharding import PartitionSpec as P

epsilon = 1e-06
MESH = pl.DeviceIdType.MESH
F32, BF16 = jnp.float32, jnp.bfloat16


def flipped(value, mask):
    bit = 1
    while bit <= mask:
        if mask & bit:
            value = value + bit * (1 - 2 * ((value // bit) % 2))
        bit *= 2
    return value


def silu(v):
    return v / (1.0 + jnp.exp(-v))


def dot(a, b):
    return jnp.dot(a, b, preferred_element_type=F32)


def kernel(
    zs, ys, tok_ref, gain_ref, routing_ref, gates_ref, wg_hbm, wu_hbm, wd_hbm, sg_hbm, su_hbm, sd_hbm,
    out_ref, buf, part, from_core, to_y, from_y, to_z, from_z, sums, wg, wu, wd, sg, su, sd,
    w_sem, agz_s, agz_r, agy_s, agy_r, agc_s, agc_r, rsc_s, rsc_r, rsy_s, rsy_r, rsz_s, rsz_r,
):
    toks, width = tok_ref.shape
    top = routing_ref.shape[0]
    lanes = buf.shape[-1] - width
    n = zs * ys * 2
    me = lax.axis_index("ep")
    c = me % 2
    y = (me // 2) % ys
    z = me // (2 * ys)
    oc, oy = 1 - c, (y + 1) % ys

    def dev(zi, yi, ci):
        return {"ep": (zi * ys + yi) * 2 + ci}

    pairs = ((sg_hbm, sg), (su_hbm, su), (sd_hbm, sd), (wg_hbm, wg), (wu_hbm, wu), (wd_hbm, wd))
    loads = [pltpu.make_async_copy(a, b, w_sem.at[i]) for i, (a, b) in enumerate(pairs)]
    for load in loads:
        load.start()

    barrier = pltpu.get_barrier_semaphore()
    gather_order = [1] + list(range(2, zs, 2))
    peers = [dev(flipped(z, k), y, c) for k in range(1, zs)] + [dev(z, oy, c), dev(z, y, oc)]
    for peer in peers:
        pl.semaphore_signal(barrier, inc=1, device_id=peer, device_id_type=MESH)

    floats = tok_ref[...].astype(F32)
    scale_inv = lax.rsqrt(jnp.mean(floats * floats, axis=-1, keepdims=True) + epsilon)
    normed = (floats * scale_inv * gain_ref[...]).astype(BF16)
    lane = lax.broadcasted_iota(jnp.int32, (toks, lanes), 1)
    tag = lax.broadcasted_iota(jnp.int32, (lanes, toks), 0)
    weight = jnp.zeros((lanes, toks), F32)
    for k in range(top):
        named = (routing_ref[k : k + 1, :] == tag) | (routing_ref[k : k + 1, :] + n == tag)
        weight = weight + jnp.where(named, gates_ref[k : k + 1, :], 0.0)
    weight = weight.T
    high = weight.astype(BF16).astype(F32)
    low = weight - high
    buf[z, c, y, :, :width] = normed
    buf[z, c, y, :, width:] = jnp.where(lane < n, high, low).astype(BF16)

    pl.semaphore_wait(barrier, len(peers))

    parts = 2 if toks % 32 == 0 else 1
    size = toks // parts
    sent = []

    def send(src, dst, s_sem, r_sem, target):
        copy = pltpu.make_async_remote_copy(
            src_ref=src, dst_ref=dst, send_sem=s_sem, recv_sem=r_sem,
            device_id=target, device_id_type=MESH,
        )
        copy.start()
        sent.append(copy)

    def piece(zi, ci, yi, h):
        return buf.at[zi, ci, yi, pl.ds(h * size, size)]

    def arrived(dst, s_sem, r_sem, source):
        pltpu.make_async_remote_copy(
            src_ref=dst, dst_ref=dst, send_sem=s_sem, recv_sem=r_sem,
            device_id=source, device_id_type=MESH,
        ).wait_recv()

    def forward_y(k, h):
        block = piece(flipped(z, k), c, y, h)
        send(block, block, agy_s.at[k, h], agy_r.at[k, h], dev(z, oy, c))

    def forward_core(k, yi, j, h):
        block = piece(flipped(z, k), c, yi, h)
        send(block, block, agc_s.at[k, j, h], agc_r.at[k, j, h], dev(z, y, oc))

    def take_z(k):
        for h in range(parts):
            block = piece(flipped(z, k), c, y, h)
            arrived(block, agz_s.at[k, h], agz_r.at[k, h], dev(flipped(z, 1 if k % 2 else k), y, c))
            if k % 2 == 0:
                send(block, block, agz_s.at[k + 1, h], agz_r.at[k + 1, h], dev(flipped(z, 1), y, c))
            forward_y(k, h)
            forward_core(k, y, 0, h)

    def take_y(k):
        for h in range(parts):
            arrived(piece(flipped(z, k), c, oy, h), agy_s.at[k, h], agy_r.at[k, h], dev(z, oy, c))
            forward_core(k, oy, 1, h)

    def experts(k):
        zi = flipped(z, k)
        for j, yi in ((0, y), (1, oy)):
            for h in range(parts):
                arrived(piece(zi, oc, yi, h), agc_s.at[k, j, h], agc_r.at[k, j, h], dev(z, y, oc))
        rows = 2 * ys * toks
        x = buf[zi, :, :, :, :width].reshape(rows, width)
        tags = buf[zi, :, :, :, width:].reshape(rows, lanes).astype(F32)
        where = lax.broadcasted_iota(jnp.int32, (rows, lanes), 1)
        mine = (where == me) | (where == me + n)
        scale = jnp.sum(jnp.where(mine, tags, 0.0), axis=-1, keepdims=True)
        hidden = (silu(dot(x, wg[0])) * dot(x, wu[0])).astype(BF16)
        outs = dot(hidden, wd[0]).astype(BF16).astype(F32) * scale
        part[zi] = outs.astype(BF16).reshape(2, ys, toks, width)
        for j, yi in ((0, oy), (1, y)):
            send(part.at[zi, oc, yi], from_core.at[k, yi], rsc_s.at[k, j], rsc_r.at[k, j], dev(z, y, oc))

    def add_core(k):
        zi = flipped(z, k)
        arrived(from_core.at[k, oy], rsc_s.at[k, 0], rsc_r.at[k, 0], dev(z, y, oc))
        for h in range(parts):
            at = pl.ds(h * size, size)
            both = part[zi, c, oy, at].astype(F32) + from_core[k, oy, at].astype(F32)
            to_y[k, at] = both.astype(BF16)
            send(to_y.at[k, at], from_y.at[k, at], rsy_s.at[k, h], rsy_r.at[k, h], dev(z, oy, c))

    def add_y(k):
        zi = flipped(z, k)
        arrived(from_core.at[k, y], rsc_s.at[k, 1], rsc_r.at[k, 1], dev(z, y, oc))
        for h in range(parts):
            at = pl.ds(h * size, size)
            arrived(from_y.at[k, at], rsy_s.at[k, h], rsy_r.at[k, h], dev(z, oy, c))
            total = part[zi, c, y, at].astype(F32) + from_core[k, y, at].astype(F32) + from_y[k, at].astype(F32)
            if k == 0:
                sums[at] = sums[at] + total
            else:
                if k % 2 and k > 1:
                    arrived(from_z.at[k - 1, at], rsz_s.at[k - 1, h], rsz_r.at[k - 1, h], dev(flipped(z, 1), y, c))
                    total = total + from_z[k - 1, at].astype(F32)
                to_z[k, at] = total.astype(BF16)
                target = dev(flipped(z, k if k % 2 else 1), y, c)
                send(to_z.at[k, at], from_z.at[k, at], rsz_s.at[k, h], rsz_r.at[k, h], target)

    for h in range(parts):
        forward_y(0, h)
        forward_core(0, y, 0, h)
    for k in gather_order:
        for h in range(parts):
            own = piece(z, c, y, h)
            send(own, own, agz_s.at[k, h], agz_r.at[k, h], dev(flipped(z, k), y, c))

    for load in loads[:3]:
        load.wait()
    x = buf[z, c, y, :, :width]
    shared_hidden = (silu(dot(x, sg[...])) * dot(x, su[...])).astype(BF16)
    sums[...] = dot(shared_hidden, sd[...])
    for load in loads[3:]:
        load.wait()

    def program():
        for k in range(1, min(zs, 3)):
            yield take_z, k
        for k in range(min(zs, 2)):
            yield take_y, k
        for i in range(zs):
            if i >= 2:
                yield add_core, i - 1
            yield experts, i
            if i + 3 < zs:
                yield take_z, i + 3
            if 1 <= i < zs - 1:
                yield take_y, i + 1
        if zs > 1:
            yield add_core, zs - 1
        yield add_core, 0
        for k in list(range(2, zs, 2)) + list(range(1, zs, 2)) + [0]:
            yield add_y, k

    for step, k in program():
        step(k)
    total = sums[...]
    for k in range(1, zs, 2):
        for h in range(parts):
            at = pl.ds(h * size, size)
            arrived(from_z.at[k, at], rsz_s.at[k, h], rsz_r.at[k, h], dev(flipped(z, k), y, c))
        total = total + from_z[k].astype(F32)
    out_ref[...] = total.astype(BF16)
    for copy in sent:
        copy.wait_send()


def body(zs, ys, *args):
    tokens, norm_gain, routing, gates, w_gate, w_up, w_down, shared_gate, shared_up, shared_down = args
    toks, width = tokens.shape
    n = zs * ys * 2
    lanes = -(-2 * n // 128) * 128
    dma = pltpu.SemaphoreType.DMA
    vmem = pl.BlockSpec(memory_space=pltpu.VMEM)
    hbm = pl.BlockSpec(memory_space=pl.ANY)
    return pl.pallas_call(
        functools.partial(kernel, zs, ys),
        out_shape=pltpu.VMEM((toks, width), BF16),
        in_specs=[vmem] * 4 + [hbm] * 6,
        out_specs=vmem,
        scratch_shapes=[
            pltpu.VMEM((zs, 2, ys, toks, width + lanes), BF16),
            pltpu.VMEM((zs, 2, ys, toks, width), BF16),
            pltpu.VMEM((zs, ys, toks, width), BF16),
            pltpu.VMEM((zs, toks, width), BF16),
            pltpu.VMEM((zs, toks, width), BF16),
            pltpu.VMEM((zs, toks, width), BF16),
            pltpu.VMEM((zs, toks, width), BF16),
            pltpu.VMEM((toks, width), F32),
        ]
        + [pltpu.VMEM(w.shape, BF16) for w in args[4:]]
        + [dma((6,))]
        + [dma((zs, 2))] * 4
        + [dma((zs, 2, 2))] * 2
        + [dma((zs, 2))] * 6,
        compiler_params=pltpu.CompilerParams(
            collective_id=0, has_side_effects=True, vmem_limit_bytes=60 * 1024 * 1024
        ),
    )(tokens, norm_gain.reshape(1, width), routing.T, gates.T, *args[4:])


def solution(mesh):
    chips = mesh.shape["ep"] // 2
    ys = 2
    zs = chips // ys
    placed = (
        P(("grp", "ep"), None),
        P(),
        P(("grp", "ep"), None),
        P(("grp", "ep"), None),
        P("ep", None, None),
        P("ep", None, None),
        P("ep", None, None),
        P(),
        P(),
        P(),
    )
    return jax.shard_map(
        functools.partial(body, zs, ys),
        mesh=mesh,
        in_specs=placed,
        out_specs=P(("grp", "ep"), None),
        check_vma=False,
    )
```

```python
import functools

import jax
import jax.numpy as jnp
from jax import lax
from jax.experimental import pallas as pl
from jax.experimental.pallas import tpu as pltpu
from jax.sharding import PartitionSpec as P

epsilon = 1e-06
MESH = pl.DeviceIdType.MESH
F32, BF16 = jnp.float32, jnp.bfloat16


def flipped(value, mask):
    bit = 1
    while bit <= mask:
        if mask & bit:
            value = value + bit * (1 - 2 * ((value // bit) % 2))
        bit *= 2
    return value


def silu(v):
    return v / (1.0 + jnp.exp(-v))


def dot(a, b):
    return jnp.dot(a, b, preferred_element_type=F32)


def kernel(
    zs, ys, tok_ref, gain_ref, routing_ref, gates_ref, wg_hbm, wu_hbm, wd_hbm, sg_hbm, su_hbm, sd_hbm,
    out_ref, buf, part, from_core, to_y, from_y, to_z, from_z, sums, wg, wu, wd, sg, su, sd,
    w_sem, agz_s, agz_r, agy_s, agy_r, agc_s, agc_r, rsc_s, rsc_r, rsy_s, rsy_r, rsz_s, rsz_r,
):
    toks, width = tok_ref.shape
    top = routing_ref.shape[0]
    lanes = buf.shape[-1] - width
    n = zs * ys * 2
    me = lax.axis_index("ep")
    c = me % 2
    y = (me // 2) % ys
    z = me // (2 * ys)
    oc, oy = 1 - c, (y + 1) % ys

    def dev(zi, yi, ci):
        return {"ep": (zi * ys + yi) * 2 + ci}

    pairs = ((sg_hbm, sg), (su_hbm, su), (sd_hbm, sd), (wg_hbm, wg), (wu_hbm, wu), (wd_hbm, wd))
    loads = [pltpu.make_async_copy(a, b, w_sem.at[i]) for i, (a, b) in enumerate(pairs)]
    for load in loads:
        load.start()

    barrier = pltpu.get_barrier_semaphore()
    gather_order = [1] + list(range(2, zs, 2))
    peers = [dev(flipped(z, k), y, c) for k in range(1, zs)] + [dev(z, oy, c), dev(z, y, oc)]
    for peer in peers:
        pl.semaphore_signal(barrier, inc=1, device_id=peer, device_id_type=MESH)

    floats = tok_ref[...].astype(F32)
    scale_inv = lax.rsqrt(jnp.mean(floats * floats, axis=-1, keepdims=True) + epsilon)
    normed = (floats * scale_inv * gain_ref[...]).astype(BF16)
    lane = lax.broadcasted_iota(jnp.int32, (toks, lanes), 1)
    tag = lax.broadcasted_iota(jnp.int32, (lanes, toks), 0)
    weight = jnp.zeros((lanes, toks), F32)
    for k in range(top):
        named = (routing_ref[k : k + 1, :] == tag) | (routing_ref[k : k + 1, :] + n == tag)
        weight = weight + jnp.where(named, gates_ref[k : k + 1, :], 0.0)
    weight = weight.T
    high = weight.astype(BF16).astype(F32)
    low = weight - high
    buf[z, c, y, :, :width] = normed
    buf[z, c, y, :, width:] = jnp.where(lane < n, high, low).astype(BF16)

    pl.semaphore_wait(barrier, len(peers))

    parts = 2 if toks % 32 == 0 else 1
    size = toks // parts
    sent = []

    def send(src, dst, s_sem, r_sem, target):
        copy = pltpu.make_async_remote_copy(
            src_ref=src, dst_ref=dst, send_sem=s_sem, recv_sem=r_sem,
            device_id=target, device_id_type=MESH,
        )
        copy.start()
        sent.append(copy)

    def piece(zi, ci, yi, h):
        return buf.at[zi, ci, yi, pl.ds(h * size, size)]

    def arrived(dst, s_sem, r_sem, source):
        pltpu.make_async_remote_copy(
            src_ref=dst, dst_ref=dst, send_sem=s_sem, recv_sem=r_sem,
            device_id=source, device_id_type=MESH,
        ).wait_recv()

    def forward_y(k, h):
        block = piece(flipped(z, k), c, y, h)
        send(block, block, agy_s.at[k, h], agy_r.at[k, h], dev(z, oy, c))

    def forward_core(k, yi, j, h):
        block = piece(flipped(z, k), c, yi, h)
        send(block, block, agc_s.at[k, j, h], agc_r.at[k, j, h], dev(z, y, oc))

    def take_z(k):
        for h in range(parts):
            block = piece(flipped(z, k), c, y, h)
            arrived(block, agz_s.at[k, h], agz_r.at[k, h], dev(flipped(z, 1 if k % 2 else k), y, c))
            if k % 2 == 0:
                send(block, block, agz_s.at[k + 1, h], agz_r.at[k + 1, h], dev(flipped(z, 1), y, c))
            forward_y(k, h)
            forward_core(k, y, 0, h)

    def take_y(k):
        for h in range(parts):
            arrived(piece(flipped(z, k), c, oy, h), agy_s.at[k, h], agy_r.at[k, h], dev(z, oy, c))
            forward_core(k, oy, 1, h)

    def experts(k):
        zi = flipped(z, k)
        for j, yi in ((0, y), (1, oy)):
            for h in range(parts):
                arrived(piece(zi, oc, yi, h), agc_s.at[k, j, h], agc_r.at[k, j, h], dev(z, y, oc))
        rows = 2 * ys * toks
        x = buf[zi, :, :, :, :width].reshape(rows, width)
        tags = buf[zi, :, :, :, width:].reshape(rows, lanes).astype(F32)
        where = lax.broadcasted_iota(jnp.int32, (rows, lanes), 1)
        mine = (where == me) | (where == me + n)
        scale = jnp.sum(jnp.where(mine, tags, 0.0), axis=-1, keepdims=True)
        hidden = (silu(dot(x, wg[0])) * dot(x, wu[0])).astype(BF16)
        outs = dot(hidden, wd[0]).astype(BF16).astype(F32) * scale
        part[zi] = outs.astype(BF16).reshape(2, ys, toks, width)
        for j, yi in ((0, oy), (1, y)):
            send(part.at[zi, oc, yi], from_core.at[k, yi], rsc_s.at[k, j], rsc_r.at[k, j], dev(z, y, oc))

    def add_core(k):
        zi = flipped(z, k)
        arrived(from_core.at[k, oy], rsc_s.at[k, 0], rsc_r.at[k, 0], dev(z, y, oc))
        for h in range(parts):
            at = pl.ds(h * size, size)
            both = part[zi, c, oy, at].astype(F32) + from_core[k, oy, at].astype(F32)
            to_y[k, at] = both.astype(BF16)
            send(to_y.at[k, at], from_y.at[k, at], rsy_s.at[k, h], rsy_r.at[k, h], dev(z, oy, c))

    def add_y(k):
        zi = flipped(z, k)
        arrived(from_core.at[k, y], rsc_s.at[k, 1], rsc_r.at[k, 1], dev(z, y, oc))
        for h in range(parts):
            at = pl.ds(h * size, size)
            arrived(from_y.at[k, at], rsy_s.at[k, h], rsy_r.at[k, h], dev(z, oy, c))
            total = part[zi, c, y, at].astype(F32) + from_core[k, y, at].astype(F32) + from_y[k, at].astype(F32)
            if k == 0:
                sums[at] = sums[at] + total
            else:
                if k % 2 and k > 1:
                    arrived(from_z.at[k - 1, at], rsz_s.at[k - 1, h], rsz_r.at[k - 1, h], dev(flipped(z, 1), y, c))
                    total = total + from_z[k - 1, at].astype(F32)
                to_z[k, at] = total.astype(BF16)
                target = dev(flipped(z, k if k % 2 else 1), y, c)
                send(to_z.at[k, at], from_z.at[k, at], rsz_s.at[k, h], rsz_r.at[k, h], target)

    for h in range(parts):
        forward_y(0, h)
        forward_core(0, y, 0, h)
    for k in gather_order:
        for h in range(parts):
            own = piece(z, c, y, h)
            send(own, own, agz_s.at[k, h], agz_r.at[k, h], dev(flipped(z, k), y, c))

    def shared(_):
        for load in loads[:3]:
            load.wait()
        x = buf[z, c, y, :, :width]
        shared_hidden = (silu(dot(x, sg[...])) * dot(x, su[...])).astype(BF16)
        sums[...] = dot(shared_hidden, sd[...])
        for load in loads[3:]:
            load.wait()

    def program():
        for k in range(1, min(zs, 3)):
            yield take_z, k
        yield shared, 0
        for k in range(min(zs, 2)):
            yield take_y, k
        for i in range(zs):
            if i >= 2:
                yield add_core, i - 1
            yield experts, i
            if i + 3 < zs:
                yield take_z, i + 3
            if 1 <= i < zs - 1:
                yield take_y, i + 1
        if zs > 1:
            yield add_core, zs - 1
        yield add_core, 0
        for k in list(range(2, zs, 2)) + list(range(1, zs, 2)) + [0]:
            yield add_y, k

    for step, k in program():
        step(k)
    total = sums[...]
    for k in range(1, zs, 2):
        for h in range(parts):
            at = pl.ds(h * size, size)
            arrived(from_z.at[k, at], rsz_s.at[k, h], rsz_r.at[k, h], dev(flipped(z, k), y, c))
        total = total + from_z[k].astype(F32)
    out_ref[...] = total.astype(BF16)
    for copy in sent:
        copy.wait_send()


def body(zs, ys, *args):
    tokens, norm_gain, routing, gates, w_gate, w_up, w_down, shared_gate, shared_up, shared_down = args
    toks, width = tokens.shape
    n = zs * ys * 2
    lanes = -(-2 * n // 128) * 128
    dma = pltpu.SemaphoreType.DMA
    vmem = pl.BlockSpec(memory_space=pltpu.VMEM)
    hbm = pl.BlockSpec(memory_space=pl.ANY)
    return pl.pallas_call(
        functools.partial(kernel, zs, ys),
        out_shape=pltpu.VMEM((toks, width), BF16),
        in_specs=[vmem] * 4 + [hbm] * 6,
        out_specs=vmem,
        scratch_shapes=[
            pltpu.VMEM((zs, 2, ys, toks, width + lanes), BF16),
            pltpu.VMEM((zs, 2, ys, toks, width), BF16),
            pltpu.VMEM((zs, ys, toks, width), BF16),
            pltpu.VMEM((zs, toks, width), BF16),
            pltpu.VMEM((zs, toks, width), BF16),
            pltpu.VMEM((zs, toks, width), BF16),
            pltpu.VMEM((zs, toks, width), BF16),
            pltpu.VMEM((toks, width), F32),
        ]
        + [pltpu.VMEM(w.shape, BF16) for w in args[4:]]
        + [dma((6,))]
        + [dma((zs, 2))] * 4
        + [dma((zs, 2, 2))] * 2
        + [dma((zs, 2))] * 6,
        compiler_params=pltpu.CompilerParams(
            collective_id=0, has_side_effects=True, vmem_limit_bytes=60 * 1024 * 1024
        ),
    )(tokens, norm_gain.reshape(1, width), routing.T, gates.T, *args[4:])


def solution(mesh):
    chips = mesh.shape["ep"] // 2
    ys = 2
    zs = chips // ys
    placed = (
        P(("grp", "ep"), None),
        P(),
        P(("grp", "ep"), None),
        P(("grp", "ep"), None),
        P("ep", None, None),
        P("ep", None, None),
        P("ep", None, None),
        P(),
        P(),
        P(),
    )
    return jax.shard_map(
        functools.partial(body, zs, ys),
        mesh=mesh,
        in_specs=placed,
        out_specs=P(("grp", "ep"), None),
        check_vma=False,
    )
```
